128 devices in a mesh: sp: 16 (over z, x), tp: 8 (over y, core).
Axes of the slice: x: 4, y: 4, z: 4, core: 2. Of those that a mesh axis runs over, the one named last changes fastest.
Arguments:
- target: bfloat16 [8192, 4096], P(('sp', 'tp')), may hold values from -0.07 to 0.07
- source: bfloat16 [16384, 4096], P(('sp', 'tp')), may hold values from -0.035 to 0.035
- gain_target: float32 [4096], replicated, may hold values from 0.1 to 1.9
- gain_source: float32 [4096], replicated, may hold values from 0.1 to 1.9
- w_query: bfloat16 [4096, 1024], P(None, 'tp'), may hold values from -1 to 1
- w_key: bfloat16 [4096, 512], replicated, may hold values from -1 to 1
- w_value: bfloat16 [4096, 512], replicated, may hold values from -0.09375 to 0.09375
- w_out: bfloat16 [1024, 4096], P('tp'), may hold values from -0.1875 to 0.1875
- grad_output: bfloat16 [8192, 4096], P(('sp', 'tp')), may hold values from -6 to 6
Outputs:
- grad_target: float32 [8192, 4096], P(('sp', 'tp'))
- grad_source: float32 [16384, 4096], P(('sp', 'tp'))
- grad_out_proj: float32 [1024, 4096], P('tp')
The draws below stay inside these ranges and needn't reach their ends.
All inputs are finite; a program needn't handle non-finite values.
Results may differ from the reference program's by a relative error of at most 0.028.
Values may be sent and summed in bfloat16 or wider, within the bound.
No kernel may reach another device: no remote copies, remote signals or barrier semaphores. Data moves between devices by JAX's collectives and lax.ppermute only.
A program may use at most 128 MiB of HBM per device.

```python
import jax
import jax.numpy as jnp
from jax import lax

D = 4096
HQ = 16
HK = 8
HD = 64
TGT_ROWS = 8192
SRC_ROWS = 16384


def aligned_draw(key):
    query_weight = jnp.clip(jax.random.normal(jax.random.fold_in(key, 11), (D, HQ * HD), jnp.float32), -6.0, 6.0) * float(D) ** (-0.5)
    key_weight = jnp.clip(jax.random.normal(jax.random.fold_in(key, 12), (D, HK * HD), jnp.float32), -6.0, 6.0) * float(D) ** (-0.5)
    target_rows = jnp.clip(jax.random.normal(jax.random.fold_in(key, 13), (TGT_ROWS, D), jnp.float32), -6.0, 6.0) * 0.01
    source_rows = jnp.clip(jax.random.normal(jax.random.fold_in(key, 14), (SRC_ROWS, D), jnp.float32), -6.0, 6.0) * 0.005
    return (query_weight, key_weight, jnp.clip(target_rows, -0.07, 0.07), jnp.clip(source_rows, -0.035, 0.035))


def draw_target(key, part):
    return aligned_draw(key)[2].astype(jnp.bfloat16)


def draw_source(key, part):
    return aligned_draw(key)[3].astype(jnp.bfloat16)


def draw_w_query(key, part):
    return aligned_draw(key)[0].astype(jnp.bfloat16)


def draw_w_key(key, part):
    return aligned_draw(key)[1].astype(jnp.bfloat16)


def block_levels(stream_key, extent, split, least, largest):
    factor_of, own = 1.0, jax.random.fold_in(stream_key, 6)
    for dim, shards_of in split:
        draws = jnp.exp(jax.random.uniform(jax.random.fold_in(own, dim), (shards_of,), jnp.float32, least / len(split), largest / len(split)))
        factor_of = factor_of * jnp.repeat(draws, extent[dim] // shards_of).reshape([-1 if axis == dim else 1 for axis in range(len(extent))])
    return factor_of


def scatter_about(rng, extent, spread, most, split=(), held_as=jnp.bfloat16):
    factor_of = block_levels(rng, extent, split, -0.22, 0.18) if split else 1.0
    array = jax.random.normal(rng, extent, jnp.float32) * spread * factor_of
    return jnp.minimum(jnp.maximum(array, -most), most).astype(held_as)


def setup_inputs(seed: int = 0) -> dict:
    streams_of = jax.random.split(jax.random.key(seed), 10)
    target = draw_target(jax.random.fold_in(streams_of[9], 71), 0)
    source = draw_source(jax.random.fold_in(streams_of[9], 71), 0)
    gain_target = jnp.clip(1.0 + 0.18 * jax.random.normal(streams_of[2], (D,), jnp.float32), 0.1, 1.9)
    gain_source = jnp.clip(1.0 + 0.18 * jax.random.normal(streams_of[3], (D,), jnp.float32), 0.1, 1.9)
    w_query = draw_w_query(jax.random.fold_in(streams_of[9], 71), 0)
    w_key = draw_w_key(jax.random.fold_in(streams_of[9], 71), 0)
    w_value = scatter_about(streams_of[6], (D, HK * HD), D ** -0.5, 0.09375)
    w_out = scatter_about(streams_of[7], (HQ * HD, D), (HQ * HD) ** -0.5, 0.1875, ((0, 8),))
    grad_output = scatter_about(streams_of[8], (TGT_ROWS, D), 1.0, 6.0, ((0, 128),))
    return dict(target=target, source=source, gain_target=gain_target, gain_source=gain_source, w_query=w_query, w_key=w_key, w_value=w_value, w_out=w_out, grad_output=grad_output)


EPS = 1e-06

def normalize(matrix, scaling):
    widened = matrix.astype(jnp.float32)
    factor = lax.rsqrt(lax.optimization_barrier(jnp.mean(widened * widened, axis=-1, keepdims=True)) + EPS)
    return (widened * factor * scaling.astype(jnp.float32)).astype(jnp.bfloat16)

def norm_back(matrix, scaling, upstream):
    widened = matrix.astype(jnp.float32)
    factor = lax.rsqrt(lax.optimization_barrier(jnp.mean(widened * widened, axis=-1, keepdims=True)) + EPS)
    weighted = upstream * scaling.astype(jnp.float32)
    inner = lax.optimization_barrier(jnp.mean(widened * weighted, axis=-1, keepdims=True))
    return factor * weighted - widened * factor * factor * factor * inner

def reference(target, source, gain_target, gain_source, w_query, w_key, w_value, w_out, grad_output):
    contract_last = (((1,), (1,)), ((), ()))
    normed_target = normalize(target, gain_target)
    normed_source = normalize(source, gain_source)
    query = jnp.dot(normed_target, w_query, preferred_element_type=jnp.float32).astype(jnp.bfloat16)
    keys_all = jnp.dot(normed_source, w_key, preferred_element_type=jnp.float32).astype(jnp.bfloat16)
    values_all = jnp.dot(normed_source, w_value, preferred_element_type=jnp.float32).astype(jnp.bfloat16)
    head_grads = lax.dot_general(grad_output, w_out, contract_last, preferred_element_type=jnp.float32).astype(jnp.bfloat16)
    target_count = target.shape[0]
    source_count = source.shape[0]
    group_size = HQ // HK
    score_scale = float(HD) ** (-0.5)
    query_heads = query.reshape(target_count, HQ, HD).transpose(1, 0, 2)
    grad_heads = head_grads.reshape(target_count, HQ, HD).transpose(1, 0, 2)
    key_heads = keys_all.reshape(source_count, HK, HD).transpose(1, 0, 2)
    value_heads = values_all.reshape(source_count, HK, HD).transpose(1, 0, 2)

    def one_head(bundle):
        query_head, grad_head, position = bundle
        key_head = key_heads[position]
        value_head = value_heads[position]
        scores = jnp.dot(query_head, key_head.T, preferred_element_type=jnp.float32) * score_scale
        maxima = lax.optimization_barrier(jnp.max(scores, axis=-1, keepdims=True))
        weights = jnp.exp(scores - maxima)
        totals = lax.optimization_barrier(jnp.sum(weights, axis=-1, keepdims=True))
        output = (jnp.dot(weights.astype(jnp.bfloat16), value_head, preferred_element_type=jnp.float32) / totals).astype(jnp.bfloat16)
        attend = weights / totals
        delta_sum = lax.optimization_barrier(jnp.sum(grad_head.astype(jnp.float32) * output.astype(jnp.float32), axis=-1, keepdims=True))
        grad_attend = jnp.dot(grad_head, value_head.T, preferred_element_type=jnp.float32)
        mixed = (attend * (grad_attend - delta_sum) * score_scale).astype(jnp.bfloat16)
        grad_query = jnp.dot(mixed, key_head, preferred_element_type=jnp.float32).astype(jnp.bfloat16)
        grad_key = jnp.dot(mixed.T, query_head, preferred_element_type=jnp.float32)
        grad_value = jnp.dot(attend.astype(jnp.bfloat16).T, grad_head, preferred_element_type=jnp.float32)
        return (output, grad_query, grad_key, grad_value)
    positions = jnp.arange(HQ, dtype=jnp.int32) // group_size
    output, grad_query, grad_key, grad_value = lax.map(one_head, (query_heads, grad_heads, positions))
    attention = output.transpose(1, 0, 2).reshape(target_count, HQ * HD)
    query_grads = grad_query.transpose(1, 0, 2).reshape(target_count, HQ * HD)
    key_grads = lax.optimization_barrier(jnp.sum(grad_key.reshape(HK, group_size, source_count, HD), axis=1)).astype(jnp.bfloat16)
    key_grads = key_grads.transpose(1, 0, 2).reshape(source_count, HK * HD)
    value_grads = lax.optimization_barrier(jnp.sum(grad_value.reshape(HK, group_size, source_count, HD), axis=1)).astype(jnp.bfloat16)
    value_grads = value_grads.transpose(1, 0, 2).reshape(source_count, HK * HD)
    grad_xn = lax.dot_general(query_grads, w_query, contract_last, preferred_element_type=jnp.float32)
    grad_target = norm_back(target, gain_target, grad_xn)
    grad_sn = lax.dot_general(key_grads, w_key, contract_last, preferred_element_type=jnp.float32)
    grad_sn = grad_sn + lax.dot_general(value_grads, w_value, contract_last, preferred_element_type=jnp.float32)
    grad_source = norm_back(source, gain_source, grad_sn)
    grad_out_proj = lax.dot_general(attention, grad_output, (((0,), (0,)), ((), ())), preferred_element_type=jnp.float32)
    return (grad_target, grad_source, grad_out_proj)
```

```python
import functools
import math

import jax
import jax.numpy as jnp
from jax import lax
from jax.experimental import pallas as pl
from jax.experimental.pallas import tpu as pltpu
from jax.sharding import Mesh
from jax.sharding import PartitionSpec as P

HD = 64
EPS = 1e-06
NZ = 4
NX = 4
BF = jnp.bfloat16
F32 = jnp.float32
NT = (((1,), (1,)), ((), ()))


def normalize(matrix, scaling):
    widened = matrix.astype(F32)
    factor = lax.rsqrt(jnp.mean(widened * widened, axis=-1, keepdims=True) + EPS)
    return (widened * factor * scaling).astype(BF)


def pairs_kernel(x_ref, g_ref, wk_ref, wv_ref, out_ref, sn):
    @pl.when(pl.program_id(0) == 0)
    def _():
        sn[...] = normalize(x_ref[...], g_ref[...])

    k = jnp.dot(sn[...], wk_ref[...], preferred_element_type=F32).astype(BF)
    v = jnp.dot(sn[...], wv_ref[...], preferred_element_type=F32).astype(BF)
    out_ref[0] = jnp.concatenate([k[:, :HD], v[:, :HD]], axis=1)
    out_ref[1] = jnp.concatenate([k[:, HD:], v[:, HD:]], axis=1)


def project_pairs(source, gain, w_key, w_value):
    rows, width = source.shape
    heads = w_key.shape[1] // HD
    return pl.pallas_call(
        pairs_kernel,
        grid=(heads // 2,),
        in_specs=[
            pl.BlockSpec((rows, width), lambda i: (0, 0)),
            pl.BlockSpec((1, width), lambda i: (0, 0)),
            pl.BlockSpec((width, 2 * HD), lambda i: (0, i)),
            pl.BlockSpec((width, 2 * HD), lambda i: (0, i)),
        ],
        out_specs=pl.BlockSpec((2, rows, 2 * HD), lambda i: (i, 0, 0)),
        out_shape=jax.ShapeDtypeStruct((heads, rows, 2 * HD), BF),
        scratch_shapes=[pltpu.VMEM((rows, width), BF)],
        name="pairs",
    )(source, gain.reshape(1, width), w_key, w_value)


def forward_kernel(qt_ref, kv_ref, o_ref, st_ref, e_ref, kvt_ref, vt1, sbuf, *, nj):
    first = (pl.program_id(0) == 0) & (pl.program_id(1) == 0)
    src = kv_ref.shape[1]

    @pl.when(first)
    def _():
        row = lax.broadcasted_iota(jnp.int32, (16, src), 0)
        ones = jnp.where(row == 0, 1.0, 0.0).astype(BF)
        for j in range(nj):
            turned = kv_ref[j].T
            kvt_ref[j] = turned
            vt1[j, 0:HD, :] = turned[HD:, :]
            vt1[j, HD:, :] = ones

    q = qt_ref[0]
    highest = None
    acc = None
    sbuf[0] = jnp.dot(kv_ref[0, :, 0:HD], q, preferred_element_type=F32)
    for j in range(nj):
        if j + 1 < nj:
            sbuf[(j + 1) % 2] = jnp.dot(kv_ref[j + 1, :, 0:HD], q, preferred_element_type=F32)
        s = sbuf[j % 2]
        top = jnp.max(s, axis=0, keepdims=True)
        new = top if highest is None else jnp.maximum(highest, top)
        e = jnp.exp2(s - new).astype(BF)
        e_ref[j, 0] = e
        part = jnp.dot(vt1[j], e, preferred_element_type=F32)
        acc = part if acc is None else acc * jnp.exp2(highest - new) + part
        highest = new
        st_ref[0, 0, j : j + 1, :] = new
    total = acc[HD : HD + 1]
    st_ref[0, 0, nj : nj + 1, :] = total
    o_ref[0] = (acc[0:HD] / total).astype(BF)


def forward(qt, kv):
    nk, width, tgt = qt.shape
    nj, src, _ = kv.shape
    nh = width // HD
    return pl.pallas_call(
        functools.partial(forward_kernel, nj=nj),
        grid=(nk, nh),
        in_specs=[
            pl.BlockSpec((1, HD, tgt), lambda k, h: (k, h, 0)),
            pl.BlockSpec((nj, src, 2 * HD), lambda k, h: (0, 0, 0)),
        ],
        out_specs=[
            pl.BlockSpec((1, HD, tgt), lambda k, h: (k, h, 0)),
            pl.BlockSpec((1, 1, 8, tgt), lambda k, h: (k, h, 0, 0)),
            pl.BlockSpec((nj, 1, src, tgt), lambda k, h: (0, k * nh + h, 0, 0)),
            pl.BlockSpec((nj, 2 * HD, src), lambda k, h: (0, 0, 0)),
        ],
        out_shape=[
            jax.ShapeDtypeStruct((nk, width, tgt), BF),
            jax.ShapeDtypeStruct((nk, nh, 8, tgt), F32),
            jax.ShapeDtypeStruct((nj, nk * nh, src, tgt), BF),
            jax.ShapeDtypeStruct((nj, 2 * HD, src), BF),
        ],
        scratch_shapes=[pltpu.VMEM((nj, HD + 16, src), BF), pltpu.VMEM((2, src, tgt), F32)],
        cost_estimate=pl.CostEstimate(
            flops=40_000_000_000, transcendentals=nj * nk * nh * src * tgt, bytes_accessed=40_000_000
        ),
        name="forward",
    )(qt, kv)


def backward_kernel(
    j0, w_ref, qt_ref, dot_ref, kv_ref, kvt_ref, e_ref, dq_in, dkv_ref, dq_ref, vaug, rhs, store
):
    j = pl.program_id(0)
    i = pl.program_id(1)
    src = kv_ref.shape[1]
    tgt = qt_ref.shape[2]

    @pl.when(i == 0)
    def _():
        lane = lax.broadcasted_iota(jnp.int32, (src, HD), 1)
        vaug[:, 0:HD] = kv_ref[0, :, HD:]
        vaug[:, HD:] = jnp.where(lane < 2, 1.0, 0.0).astype(BF)

    @pl.when((i == 0) & (j == 0))
    def _():
        rhs[...] = jnp.zeros_like(rhs)

    share = w_ref[0, 0, pl.ds(j + j0, 1), :]
    delta = w_ref[0, 0, 4:5, :] * share
    high = delta.astype(BF).astype(F32)
    low = delta - high
    dos = (dot_ref[0].astype(F32) * share).astype(BF)
    rhs[0:HD, :] = dos
    row = lax.broadcasted_iota(jnp.int32, (16, tgt), 0)
    rhs[HD : HD + 16, :] = jnp.where(row == 0, -high, jnp.where(row == 1, -low, 0.0)).astype(BF)
    dp = jnp.dot(vaug[...], rhs[...], preferred_element_type=F32)
    e = e_ref[0, 0]
    g = e * dp.astype(BF)
    dv = lax.dot_general(dos, e, NT, preferred_element_type=F32)
    dk = lax.dot_general(qt_ref[0], g, NT, preferred_element_type=F32)

    @pl.when(i == 0)
    def _():
        store[0:HD, :] = dk
        store[HD:, :] = dv

    @pl.when(i > 0)
    def _():
        store[0:HD, :] += dk
        store[HD:, :] += dv

    @pl.when(i == pl.num_programs(1) - 1)
    def _():
        row = lax.broadcasted_iota(jnp.int32, (2 * HD, 1), 0)
        scale = jnp.where(row < HD, math.log(2.0), 1.0)
        dkv_ref[0] = (store[...] * scale).T.astype(dkv_ref.dtype)

    dq = jnp.dot(kvt_ref[0, 0:HD, :], g, preferred_element_type=F32)

    @pl.when(j == 0)
    def _():
        dq_ref[i] = dq_in[i] + dq

    @pl.when(j > 0)
    def _():
        dq_ref[i] += dq


def backward(w, qt, dot, kv, kvt, e, dq_in, j0, njc, dtype):
    nk, width, tgt = qt.shape
    src = kv.shape[1]
    nh = width // HD
    nb = nk * nh
    return pl.pallas_call(
        functools.partial(backward_kernel, j0),
        grid=(njc, nb),
        in_specs=[
            pl.BlockSpec((1, 1, 8, tgt), lambda j, i: (i // nh, i % nh, 0, 0)),
            pl.BlockSpec((1, HD, tgt), lambda j, i: (i // nh, i % nh, 0)),
            pl.BlockSpec((1, HD, tgt), lambda j, i: (i // nh, i % nh, 0)),
            pl.BlockSpec((1, src, 2 * HD), lambda j, i: (j + j0, 0, 0)),
            pl.BlockSpec((1, 2 * HD, src), lambda j, i: (j + j0, 0, 0)),
            pl.BlockSpec((1, 1, src, tgt), lambda j, i: (j + j0, i, 0, 0)),
            pl.BlockSpec((nb, HD, tgt), lambda j, i: (0, 0, 0)),
        ],
        out_specs=[
            pl.BlockSpec((1, src, 2 * HD), lambda j, i: (j, 0, 0)),
            pl.BlockSpec((nb, HD, tgt), lambda j, i: (0, 0, 0)),
        ],
        out_shape=[
            jax.ShapeDtypeStruct((njc, src, 2 * HD), dtype),
            jax.ShapeDtypeStruct((nb, HD, tgt), F32),
        ],
        scratch_shapes=[
            pltpu.VMEM((src, 2 * HD), BF),
            pltpu.VMEM((2 * HD, tgt), BF),
            pltpu.VMEM((2 * HD, src), F32),
        ],
        cost_estimate=pl.CostEstimate(
            flops=17_000_000_000 * njc, transcendentals=0, bytes_accessed=9_000_000 * njc
        ),
        name="backward%d" % j0,
    )(w, qt, dot, kv, kvt, e, dq_in)


def norm_back(x, scaling, upstream):
    widened = x.astype(F32)
    factor = lax.rsqrt(jnp.mean(widened * widened, axis=-1, keepdims=True) + EPS)
    weighted = upstream * scaling
    inner = jnp.mean(widened * weighted, axis=-1, keepdims=True)
    return factor * weighted - widened * factor * factor * factor * inner


def source_kernel(dkv_ref, wk_ref, wv_ref, x_ref, g_ref, out_ref, dk, dv, dsn):
    i = pl.program_id(0)
    heads = dkv_ref.shape[0]
    cols = wk_ref.shape[0]

    @pl.when(i == 0)
    def _():
        for h in range(heads):
            dk[:, h * HD : (h + 1) * HD] = dkv_ref[h, :, :HD]
            dv[:, h * HD : (h + 1) * HD] = dkv_ref[h, :, HD:]

    part = lax.dot_general(dk[...], wk_ref[...], NT, preferred_element_type=F32)
    part = part + lax.dot_general(dv[...], wv_ref[...], NT, preferred_element_type=F32)
    dsn[:, pl.ds(pl.multiple_of(i * cols, cols), cols)] = part

    @pl.when(i == pl.num_programs(0) - 1)
    def _():
        out_ref[...] = norm_back(x_ref[...], g_ref[...], dsn[...])


def source_grad(dkv, w_key, w_value, source, gain):
    heads, rows, _ = dkv.shape
    width = source.shape[1]
    steps = 8
    cols = width // steps
    return pl.pallas_call(
        source_kernel,
        grid=(steps,),
        in_specs=[
            pl.BlockSpec((heads, rows, 2 * HD), lambda i: (0, 0, 0)),
            pl.BlockSpec((cols, heads * HD), lambda i: (i, 0)),
            pl.BlockSpec((cols, heads * HD), lambda i: (i, 0)),
            pl.BlockSpec((rows, width), lambda i: (0, 0)),
            pl.BlockSpec((1, width), lambda i: (0, 0)),
        ],
        out_specs=pl.BlockSpec((rows, width), lambda i: (0, 0)),
        out_shape=jax.ShapeDtypeStruct((rows, width), F32),
        scratch_shapes=[
            pltpu.VMEM((rows, heads * HD), BF),
            pltpu.VMEM((rows, heads * HD), BF),
            pltpu.VMEM((rows, width), F32),
        ],
        name="source_grad",
    )(dkv, w_key, w_value, source, gain.reshape(1, width))


def target_kernel(dq_ref, wq_ref, x_ref, g_ref, out_ref, dxn):
    i = pl.program_id(0)
    parts = dq_ref.shape[0]
    cols = wq_ref.shape[1]
    part = None
    for t in range(parts):
        one = lax.dot_general(dq_ref[t], wq_ref[t], NT, preferred_element_type=F32)
        part = one if part is None else part + one
    dxn[:, pl.ds(pl.multiple_of(i * cols, cols), cols)] = part

    @pl.when(i == pl.num_programs(0) - 1)
    def _():
        out_ref[...] = norm_back(x_ref[...], g_ref[...], dxn[...])


def target_grad(dq, w_all, target, gain):
    parts, rows, part_width = dq.shape
    width = target.shape[1]
    steps = 8
    cols = width // steps
    return pl.pallas_call(
        target_kernel,
        grid=(steps,),
        in_specs=[
            pl.BlockSpec((parts, rows, part_width), lambda i: (0, 0, 0)),
            pl.BlockSpec((parts, cols, part_width), lambda i: (0, i, 0)),
            pl.BlockSpec((rows, width), lambda i: (0, 0)),
            pl.BlockSpec((1, width), lambda i: (0, 0)),
        ],
        out_specs=pl.BlockSpec((rows, width), lambda i: (0, 0)),
        out_shape=jax.ShapeDtypeStruct((rows, width), F32),
        scratch_shapes=[pltpu.VMEM((rows, width), F32)],
        name="target_grad",
    )(dq, w_all, target, gain.reshape(1, width))


def take_from(a, axis, size, shift):
    return lax.ppermute(a, axis, [((i + shift) % size, i) for i in range(size)])


def give_to(a, axis, size, shift):
    return lax.ppermute(a, axis, [(i, (i + shift) % size) for i in range(size)])


def gathered(a, axis, size):
    return jnp.stack([a] + [take_from(a, axis, size, k) for k in range(1, size)])


def turned(a, shift):
    return a if shift == 0 else jnp.concatenate([a[-shift:], a[:-shift]])


def shards(target, source, gain_target, gain_source, w_query, w_key, w_value, w_out, grad_output):
    across = lax.axis_size("tp")
    local = target.shape[0]
    width = target.shape[1]

    normed_target = normalize(target, gain_target)
    all_target = lax.all_gather(normed_target, "tp", axis=0, tiled=True)
    pairs = project_pairs(source, gain_source, w_key, w_value)
    own_pairs = lax.all_to_all(pairs, "tp", split_axis=0, concat_axis=0, tiled=True)
    kv = gathered(own_pairs.reshape(-1, 2 * HD), "x", NX)

    score_scale = math.log2(math.e) / math.sqrt(HD)
    own_qt = lax.dot_general(
        w_query, all_target, (((0,), (1,)), ((), ())), preferred_element_type=F32
    )
    own_qt = (own_qt * score_scale).astype(BF)
    qt = gathered(own_qt, "z", NZ)

    grad_output, _ = lax.optimization_barrier((grad_output, all_target))
    all_grad = lax.all_gather(grad_output, "tp", axis=0, tiled=True)
    own_dot = lax.dot_general(w_out, all_grad, NT, preferred_element_type=F32).astype(BF)
    dot = gathered(own_dot, "z", NZ)

    w_first, _ = lax.optimization_barrier((w_query, all_grad))
    w_all = lax.all_gather(w_first, "tp", axis=0, tiled=False)

    o_part, stats, e, kvt = forward(qt, kv)
    nk, wide, tgt = qt.shape
    nh = wide // HD

    def by_head(a):
        return a.astype(F32).reshape(nk, nh, HD, tgt)

    delta_part = jnp.sum(by_head(dot) * by_head(o_part), axis=2)
    top_part, sum_part = stats[:, :, NX - 1], stats[:, :, NX]
    small = jnp.stack([top_part, sum_part, delta_part], axis=1)
    smalls = [small] + [turned(take_from(small, "z", NZ, s), s) for s in range(1, NZ)]
    top = functools.reduce(jnp.maximum, [s[:, 0] for s in smalls])
    shares = [jnp.exp2(s[:, 0] - top) * s[:, 1] for s in smalls]
    total = sum(shares)
    delta = sum(w * s[:, 2] for w, s in zip(shares, smalls)) / total
    chunk_share = jnp.exp2(stats[:, :, 0:NX] - top[:, :, None]) / total[:, :, None]
    weights = jnp.concatenate(
        [chunk_share, delta[:, :, None], jnp.zeros((nk, nh, 3, tgt), F32)], axis=2
    )

    o = 0.0
    for k in range(NZ):
        got = o_part[0] if k == 0 else give_to(o_part[k], "z", NZ, k)
        part_share = shares[(NZ - k) % NZ][0] / total[0]
        o = o + got.astype(F32).reshape(nh, HD, tgt) * part_share[:, None]
    o = o.astype(BF).reshape(wide, tgt)
    proj_part = lax.dot_general(
        o, all_grad, (((1,), (0,)), ((), ())), preferred_element_type=F32
    ).astype(BF)
    grad_out_proj = lax.psum(proj_part, ("z", "x")).astype(F32)

    dq_zero = jnp.zeros((nk * nh, HD, tgt), F32)
    dkv_far, dq_far = backward(weights, qt, dot, kv, kvt, e, dq_zero, 1, NX - 1, BF)
    dkv_got = [give_to(dkv_far[j - 1], "x", NX, j) for j in range(1, NX)]
    dkv_own, dq_all = backward(weights, qt, dot, kv, kvt, e, dq_far, 0, 1, F32)

    dq_all = (dq_all * (1.0 / math.sqrt(HD))).reshape(nk, wide, tgt)
    dq_got = [give_to(dq_all[k].astype(BF), "z", NZ, k) for k in range(1, NZ)]

    dkv = dkv_own[0] + sum(d.astype(F32) for d in dkv_got)
    dkv = dkv.astype(BF).reshape(across, -1, 2 * HD)
    dkv = lax.all_to_all(dkv, "tp", split_axis=0, concat_axis=0, tiled=True)
    grad_source = source_grad(dkv, w_key, w_value, source, gain_source)

    dq = dq_all[0] + sum(d.astype(F32) for d in dq_got)
    dq = dq.T.astype(BF).reshape(across, local, wide)
    dq = lax.all_to_all(dq, "tp", split_axis=0, concat_axis=0, tiled=True)
    grad_target = target_grad(dq, w_all, target, gain_target)
    return (grad_target, grad_source, grad_out_proj)


def solution(mesh):
    fine = Mesh(mesh.devices.reshape(NZ, NX, -1), ("z", "x", "tp"))
    rows = P(("z", "x", "tp"), None)
    return jax.shard_map(
        shards,
        mesh=fine,
        in_specs=(rows, rows, P(), P(), P(None, "tp"), P(), P(), P("tp", None), rows),
        out_specs=(rows, rows, P("tp", None)),
        check_vma=False,
    )
```
